32 devices in a mesh: sp: 4 (over y, x), tp: 8 (over z, core).
Axes of the slice: x: 2, y: 2, z: 4, core: 2. Of those that a mesh axis runs over, the one named last changes fastest.
Arguments:
- out_gate: bfloat16 [2048, 2048], P('sp', 'tp'), may hold values from -6 to 6
- in_gate: bfloat16 [2048, 2048], P('sp', 'tp'), may hold values from -6 to 6
- conv_input: bfloat16 [2048, 2048], P('sp', 'tp'), may hold values from -6 to 6
- conv_taps: bfloat16 [3, 2048], P(None, 'tp'), may hold values from -3.5 to 3.5
- documents: int32 [2048], P('sp'), may hold values from 0 to 2, never falling along the last dimension, each value on 1 to 1536 neighbouring positions
- out_weight: bfloat16 [2048, 2048], P('tp'), may hold values from -0.125 to 0.125
- residual: bfloat16 [2048, 2048], P(('sp', 'tp')), may hold values from -6 to 6
- norm_gain: bfloat16 [2048], replicated, may hold values from 0.099609375 to 1.8984375
- expert_ids: int32 [2048, 2], P(('sp', 'tp')), may hold values from 0 to 3, all different within a row; in each aligned block of 64 rows (0 to 63, 64 to 127, ...) at most 48 rows name the same one
- route_weights: float32 [2048, 2], P(('sp', 'tp')), may hold values from 0.1 to 1
- gate_weight: bfloat16 [4, 2048, 4096], P('sp', None, 'tp'), may hold values from -0.125 to 0.125
- up_weight: bfloat16 [4, 2048, 4096], P('sp', None, 'tp'), may hold values from -0.125 to 0.125
- down_weight: bfloat16 [4, 4096, 2048], P('sp', 'tp'), may hold values from -0.09375 to 0.09375
Outputs:
- layer_out: bfloat16 [2048, 2048], P(('sp', 'tp'))
The draws below stay inside these ranges and needn't reach their ends.
Inputs may be any that keep to these rules, and one draw needn't show every extreme that they name: `expert_ids`: A token's two experts differ; in each aligned block of 64 rows no expert is named by more than 48 entries, a bound that some block reaches. `documents`: document numbers never fall along the sequence; a document holds at most 1536 positions.
All inputs are finite; a program needn't handle non-finite values.
Results may differ from the reference program's by a relative error of at most 0.017.
Values may be sent and summed in bfloat16 or wider, within the bound.
A program may use at most 64 MiB of HBM per device.

```python
import math
import jax
import jax.numpy as jnp
import numpy as np
from jax import lax

D = 2048
F = 4096
TAPS = 3
TOK_DEV = 512
TOKENS = 2048
EXPERTS = 4
ROWS = 64
CAP = 48
N_SP = 4
N_TP = 8


def steps_of(own_key, extent, split, low, top_value):
    level = 1.0
    for axis_at, blocks in split:
        draws = jax.random.uniform(jax.random.fold_in(jax.random.fold_in(own_key, 6), axis_at), (blocks,), jnp.float32, low / len(split), top_value / len(split))
        level = level * jnp.repeat(jnp.exp(draws), extent[axis_at] // blocks).reshape((-1,) + (1,) * (len(extent) - 1 - axis_at))
    return level


def profile(number_of, total, bound, skew):
    loads = [(1 << 20) // math.isqrt(rank ** skew) + 1 for rank in range(2, number_of + 1)]
    rest, counts = total - bound - (number_of - 1), [1] * (number_of - 1)
    while rest > 0:
        free = [i for i in range(number_of - 1) if counts[i] < bound]
        pool, left = sum([loads[i] for i in free]), rest
        for i in free:
            extra = min(bound - counts[i], max(1, left * loads[i] // pool), rest)
            counts[i] = counts[i] + extra
            rest = rest - extra
    return np.array([bound] + counts)


def uneven(stream_key, number_of, total, most, lean):
    if number_of == 2:
        one = jax.random.randint(stream_key, (), max(1, total - most), min(most, total - 1) + 1)
        return jnp.stack([one, total - one])
    sizes = jnp.asarray(profile(number_of, total, most, lean), jnp.int32)
    couples = (number_of - 1) // 2
    source_of, taker = sizes[1:1 + 2 * couples:2], sizes[2:2 + 2 * couples:2]
    margin = jnp.minimum(source_of - 1, most - taker)
    shifted = jax.random.randint(jax.random.fold_in(stream_key, 1), (couples,), 0, 1 << 20) % (margin + 1)
    sizes = sizes.at[1:1 + 2 * couples:2].set(source_of - shifted).at[2:2 + 2 * couples:2].set(taker + shifted)
    return sizes[jax.random.permutation(jax.random.fold_in(stream_key, 2), number_of)]


def shared_out(key, own, number, rows, count, top, bound, lean):
    ranking = jax.random.permutation(key, count)
    packed, usual = shares(count, rows * top, bound, lean, True), shares(count, rows * top, bound, lean, False)
    places = jnp.arange(count)

    def named(tallies, rotation):
        used = int((tallies > 0).sum())
        fixed = max(1, used // 4)
        passed = fixed + (places - fixed + rotation * (used - fixed)) % max(1, count - fixed)
        return jnp.zeros((count,), jnp.int32).at[ranking[jnp.where(places < fixed, places, passed)]].set(jnp.asarray(tallies, jnp.int32))

    tallies = jnp.where(number % 4 == 0, named(packed, number // 4), named(usual, number - number // 4 - 1))
    mixed = jax.random.permutation(jax.random.fold_in(own, 3), count)
    source_of, taker = mixed[0:count // 2 * 2:2], mixed[1:count // 2 * 2:2]
    slack = jnp.minimum(tallies[source_of] - 1, bound - tallies[taker]) // 2
    slack = jnp.where((source_of == ranking[0]) | (taker == ranking[0]) | (tallies[taker] == 0), 0, jnp.maximum(slack, 0))
    passed = jax.random.randint(jax.random.fold_in(own, 4), (count // 2,), 0, 1 << 20) % (slack + 1)
    tallies = tallies.at[source_of].add(-passed).at[taker].add(passed)
    labels = jnp.searchsorted(jnp.cumsum(tallies), jnp.arange(rows * top), side="right").astype(jnp.int32)
    table = labels.reshape(top, rows).T
    table = table[jax.random.permutation(jax.random.fold_in(own, 1), rows)]
    rotation = jax.random.randint(jax.random.fold_in(own, 2), (rows, 1), 0, top)
    return jnp.take_along_axis(table, (jnp.arange(top)[None, :] + rotation) % top, axis=1)


def shares(number_of, total, limit, lean, full):
    weights = [(1 << 20) // math.isqrt(grade ** lean) + 1 for grade in range(1, number_of + 1)]
    largest = limit if full else min(limit, max(-(-total // number_of), total * weights[0] // sum(weights)))
    least = 1 if total - largest >= number_of - 1 else 0
    counts, spare = [largest] + [least] * (number_of - 1), total - largest - least * (number_of - 1)
    while spare > 0:
        free = [i for i in range(1, number_of) if counts[i] < largest] or [i for i in range(1, number_of) if counts[i] < limit]
        whole, budget = sum([weights[i] for i in free]), spare
        for i in free:
            addition = min(limit - counts[i], max(1, budget * weights[i] // whole), spare)
            counts[i] = counts[i] + addition
            spare = spare - addition
    return np.array(counts)


def noise(key, shape, deviation, most, pieces=(), kind=jnp.bfloat16):
    gain = steps_of(key, shape, pieces, -0.22, 0.18) if pieces else 1.0
    array = jax.random.normal(key, shape, jnp.float32) * deviation * gain
    return jnp.minimum(jnp.maximum(array, -most), most).astype(kind)


def setup_inputs(seed: int = 0) -> dict:
    streams_of = jax.random.split(jax.random.key(seed), 14)
    out_gate = noise(streams_of[0], (TOKENS, D), 1.0, 6.0, ((0, 4), (1, 8)))
    in_gate = noise(streams_of[1], (TOKENS, D), 1.0, 6.0, ((0, 4), (1, 8)))
    conv_input = noise(streams_of[2], (TOKENS, D), 1.0, 6.0, ((0, 4), (1, 8)))
    conv_taps = noise(streams_of[3], (TAPS, D), TAPS ** -0.5, 3.5, ((1, 8),))
    documents = jnp.searchsorted(jnp.cumsum(uneven(streams_of[4], N_SP // 2 + 1, TOKENS, 3 * TOK_DEV, 0)), jnp.arange(TOKENS), side="right").astype(jnp.int32)
    out_weight = noise(streams_of[5], (D, D), D ** -0.5, 0.125, ((0, 8),))
    residual = noise(streams_of[6], (TOKENS, D), 1.0, 6.0, ((0, 32),))
    norm_gain = jnp.clip(1.0 + 0.18 * jax.random.normal(streams_of[7], (D,), jnp.float32), 0.099609375, 1.8984375).astype(jnp.bfloat16)
    expert_ids_keys = jax.random.split(jax.random.fold_in(streams_of[8], 1), TOKENS // ROWS)
    expert_ids_turns = jax.random.permutation(jax.random.fold_in(streams_of[8], 3), TOKENS // ROWS)
    expert_ids = jax.vmap(lambda own, number: shared_out(jax.random.fold_in(streams_of[8], 2), own, number, ROWS, EXPERTS, 2, CAP, 2))(expert_ids_keys, expert_ids_turns).reshape((TOKENS, 2))
    route_weights = jnp.clip(0.1 + 0.9 * jax.random.uniform(streams_of[9], (TOKENS, 2), jnp.float32) ** steps_of(streams_of[9], (TOKENS, 2), ((0, 32),), -0.2, 0.2), 0.1, 1.0)
    gate_weight = noise(streams_of[10], (EXPERTS, D, F), D ** -0.5, 0.125, ((0, 4), (2, 8)))
    up_weight = noise(streams_of[11], (EXPERTS, D, F), D ** -0.5, 0.125, ((0, 4), (2, 8)))
    down_weight = noise(streams_of[12], (EXPERTS, F, D), F ** -0.5, 0.09375, ((0, 4), (1, 8)))
    return dict(out_gate=out_gate, in_gate=in_gate, conv_input=conv_input, conv_taps=conv_taps, documents=documents, out_weight=out_weight, residual=residual, norm_gain=norm_gain, expert_ids=expert_ids, route_weights=route_weights, gate_weight=gate_weight, up_weight=up_weight, down_weight=down_weight)


EPS = 1e-06

def slot_index(expert_ids, experts, capacity):
    listed = expert_ids.reshape(-1).astype(jnp.int32)
    onehot = (listed[:, None] == jnp.arange(experts, dtype=jnp.int32)[None, :]).astype(jnp.int32)
    earlier = (jnp.cumsum(onehot, axis=0) - onehot).astype(jnp.int32)
    within = lax.optimization_barrier(jnp.sum(earlier * onehot, axis=1)).astype(jnp.int32)
    return (listed * capacity + within).astype(jnp.int32)

def dispatch_block(target, block_rows):
    count = block_rows.shape[0]
    slots = jnp.arange(EXPERTS * CAP, dtype=jnp.int32)
    table = lax.optimization_barrier(jnp.sum((target.reshape(count, 2)[:, :, None] == slots[None, None, :]).astype(jnp.float32), axis=1))
    placed = lax.dot_general(table, block_rows.astype(jnp.float32), (((0,), (0,)), ((), ())))
    return placed.astype(jnp.bfloat16)

def run_expert(operands):
    expert_in, gate_part, up_part, down_part = operands
    gate_proj = jnp.dot(expert_in, gate_part, preferred_element_type=jnp.float32)
    up_proj = jnp.dot(expert_in, up_part, preferred_element_type=jnp.float32)
    act = (jax.nn.silu(gate_proj) * up_proj).astype(jnp.bfloat16)
    width = F // N_TP

    def add_block(total, index):
        columns = lax.dynamic_slice_in_dim(act, index * width, width, 1)
        weight_rows = lax.dynamic_slice_in_dim(down_part, index * width, width, 0)
        partial_sum = lax.optimization_barrier(jnp.dot(columns, weight_rows, preferred_element_type=jnp.float32).astype(jnp.bfloat16))
        return (total + partial_sum.astype(jnp.float32), None)
    total, ignored = lax.scan(add_block, jnp.zeros((expert_in.shape[0], D), jnp.float32), jnp.arange(N_TP, dtype=jnp.int32))
    return total.astype(jnp.bfloat16)

def reference(out_gate, in_gate, conv_input, conv_taps, documents, out_weight, residual, norm_gain, expert_ids, route_weights, gate_weight, up_weight, down_weight):
    length = conv_input.shape[0]
    signal = in_gate.astype(jnp.float32) * conv_input.astype(jnp.float32)
    tap_values = conv_taps.astype(jnp.float32)
    position = jnp.arange(length, dtype=jnp.int32)
    mixed_conv = tap_values[2][None, :] * signal
    for offset in (1, 2):
        earlier_signal = jnp.pad(signal, ((offset, 0), (0, 0)))[:length]
        earlier_docs = jnp.pad(documents, (offset, 0))[:length]
        allowed = (position >= offset) & (earlier_docs == documents)
        mixed_conv = mixed_conv + jnp.where(allowed[:, None], tap_values[2 - offset][None, :] * earlier_signal, 0.0)
    gated = (out_gate.astype(jnp.float32) * mixed_conv).astype(jnp.bfloat16)
    width = D // N_TP

    def add_block(total, index):
        columns = lax.dynamic_slice_in_dim(gated, index * width, width, 1)
        weight_rows = lax.dynamic_slice_in_dim(out_weight, index * width, width, 0)
        partial_sum = lax.optimization_barrier(jnp.dot(columns, weight_rows, preferred_element_type=jnp.float32).astype(jnp.bfloat16))
        return (total + partial_sum.astype(jnp.float32), None)
    mixed, ignored = lax.scan(add_block, jnp.zeros((length, D), jnp.float32), jnp.arange(N_TP, dtype=jnp.int32))
    hidden_state = (residual.astype(jnp.float32) + mixed).astype(jnp.bfloat16)
    hidden_wide = hidden_state.astype(jnp.float32)
    stats = lax.optimization_barrier(jnp.mean(hidden_wide * hidden_wide, axis=-1, keepdims=True))
    normed = (hidden_wide * lax.rsqrt(stats + EPS) * norm_gain.astype(jnp.float32)[None, :]).astype(jnp.bfloat16)
    block_count = N_SP * N_TP
    normed_blocks = normed.reshape(block_count, ROWS, D)
    route_blocks = expert_ids.reshape(block_count, ROWS, 2)
    targets = jax.vmap(lambda ids: slot_index(ids, EXPERTS, CAP))(route_blocks)
    buffers = jax.vmap(dispatch_block)(targets, normed_blocks)
    expert_rows = buffers.reshape(block_count, EXPERTS, CAP, D).transpose(1, 0, 2, 3).reshape(EXPERTS, block_count * CAP, D)
    expert_out = lax.map(run_expert, (expert_rows, gate_weight, up_weight, down_weight))
    returned = expert_out.reshape(EXPERTS, block_count, CAP, D).transpose(1, 0, 2, 3).reshape(block_count, EXPERTS * CAP, D)
    picked = jax.vmap(lambda table, target: table[target])(returned, targets)
    picked = picked.astype(jnp.float32).reshape(block_count, ROWS, 2, D)
    weights = route_weights.astype(jnp.float32).reshape(block_count, ROWS, 2)
    combined = lax.optimization_barrier(jnp.sum(picked * weights[:, :, :, None], axis=2)).reshape(length, D)
    return (hidden_wide + combined).astype(jnp.bfloat16)
```

```python
import functools

import jax
import jax.numpy as jnp
from jax import lax
from jax.experimental import pallas as pl
from jax.experimental.pallas import tpu as pltpu
from jax.sharding import PartitionSpec as P

EPS = 1e-06


def passed_along(block, axis, distance):
    devices = range(lax.axis_size(axis))
    route = [(i - distance, i) for i in devices if i - distance in devices]
    return lax.ppermute(block, axis, route)


MESH = pl.DeviceIdType.MESH
CHUNK = 16
COLS = 512


def where_am_i(n_sp, nz):
    s, t = lax.axis_index("sp"), lax.axis_index("tp")
    z, c = t // 2, t % 2
    return s, z, c


def greet(s, z, c, n_sp, nz):
    barrier = pltpu.get_barrier_semaphore()
    peers = [(s, 2 * z + 1 - c)]
    peers += [(s, 2 * lax.rem(z + i, nz) + c) for i in range(1, nz)]
    peers += [(lax.rem(s + k, n_sp), 2 * z + c) for k in range(1, n_sp)]
    for peer in peers:
        pl.semaphore_signal(barrier, inc=1, device_id=peer, device_id_type=MESH)
    pl.semaphore_wait(barrier, len(peers))


def send(src, dst, send_sem, recv_sem, peer):
    copy = pltpu.make_async_remote_copy(
        src_ref=src,
        dst_ref=dst,
        send_sem=send_sem,
        recv_sem=recv_sem,
        device_id=peer,
        device_id_type=MESH,
    )
    copy.start()
    return copy


def by_rows(rows, body):
    def step(r, carry):
        body(pl.ds(pl.multiple_of(r * CHUNK, CHUNK), CHUNK))
        return carry

    lax.fori_loop(0, rows // CHUNK, step, 0)


def by_columns(width, body):
    def step(r, carry):
        body(pl.ds(pl.multiple_of(r * COLS, COLS), COLS))
        return carry

    lax.fori_loop(0, width // COLS, step, 0)


def slot_hits(meta, s, n_sp, cap):
    rows = meta.shape[1]
    slots = lax.broadcasted_iota(jnp.int32, (n_sp * cap, rows), 0).astype(jnp.float32)
    own = s.astype(jnp.float32)
    hits = []
    for k in range(2):
        ahead = meta[2 * k : 2 * k + 1, :] - own
        ahead = jnp.where(ahead < 0.0, ahead + float(n_sp), ahead)
        hits.append(slots == ahead * float(cap) + meta[2 * k + 1 : 2 * k + 2, :])
    return hits


def dispatch_kernel(
    n_sp, nz, cap, part, residual, gain, meta, hidden, metas, gathered,
    rx, stage, rz, nbuf, routed,
    d_send, d_recv, m_send, m_recv, z_send, z_recv, n_send, n_recv, p_send, p_recv, f_send, f_recv,
):
    s, z, c = where_am_i(n_sp, nz)
    o = 1 - c
    partner = (s, 2 * z + o)
    rows, width = residual.shape
    order = list(range(1, nz)) + [0]
    ahead = [lax.rem(z + i, nz) for i in range(nz)]
    greet(s, z, c, n_sp, nz)

    halves = {}
    for i in order:
        halves[i] = send(part.at[ahead[i], o], rx.at[i], d_send.at[i], d_recv.at[i], partner)
    notes = [send(meta, metas.at[i], m_send.at[i], m_recv.at[i], (s, 2 * ahead[i] + c)) for i in range(1, nz)]
    metas[0] = meta[...]

    sums = []
    for i in order:
        halves[i].wait_recv()
        if i:

            def add(r, i=i):
                stage[i, r, :] = (
                    part[ahead[i], c, r, :].astype(jnp.float32) + rx[i, r, :].astype(jnp.float32)
                ).astype(jnp.bfloat16)

            by_rows(rows, add)
            sums.append(send(stage.at[i], rz.at[i], z_send.at[i], z_recv.at[i], (s, 2 * ahead[i] + c)))
    for copy in sums:
        copy.wait_recv()

    def norm(r):
        total = part[z, c, r, :].astype(jnp.float32) + rx[0, r, :].astype(jnp.float32)
        for i in range(1, nz):
            total = total + rz[i, r, :].astype(jnp.float32)
        state = (residual[r, :].astype(jnp.float32) + total).astype(jnp.bfloat16)
        hidden[r, :] = state
        wide = state.astype(jnp.float32)
        stats = jnp.mean(wide * wide, axis=-1, keepdims=True)
        nbuf[0, r, :] = (wide * lax.rsqrt(stats + EPS) * gain[...].astype(jnp.float32)).astype(jnp.bfloat16)

    by_rows(rows, norm)
    spread = [
        send(nbuf.at[0], nbuf.at[i], n_send.at[i], n_recv.at[i], (s, 2 * ahead[i] + c)) for i in range(1, nz)
    ]

    sent, forwards = [], []

    def forward(i):
        for copy in sent[i]:
            copy.wait_recv()
        forwards.append(send(gathered.at[i, 0], gathered.at[i, 1], f_send.at[i], f_recv.at[i], partner))

    for i in range(nz):
        if i:
            notes[i - 1].wait_recv()
            spread[i - 1].wait_recv()
        first, second = slot_hits(metas[i], s, n_sp, cap)
        table = (first | second).astype(jnp.float32).astype(jnp.bfloat16)

        def place(cols, i=i, table=table):
            placed = jnp.dot(table, nbuf[i, :, cols], preferred_element_type=jnp.float32).astype(jnp.bfloat16)
            gathered[i, 0, 0, :, cols] = placed[:cap]
            for k in range(1, n_sp):
                routed[i, k, :, cols] = placed[k * cap : (k + 1) * cap]

        by_columns(width, place)
        sent.append([
            send(
                routed.at[i, k], gathered.at[i, 0, k], p_send.at[i, k], p_recv.at[i, k],
                (lax.rem(s + k, n_sp), 2 * z + c),
            )
            for k in range(1, n_sp)
        ])
        if i:
            forward(i - 1)
    forward(nz - 1)
    for copy in forwards:
        copy.wait_recv()
    for copy in list(halves.values()) + notes + sums + spread + sum(sent, []) + forwards:
        copy.wait_send()


def return_kernel(
    n_sp, nz, cap, partial, hidden, metas, out,
    rx, stage, arrived, mine, combined, zrx,
    d_send, d_recv, p_send, p_recv, z_send, z_recv,
):
    s, z, c = where_am_i(n_sp, nz)
    partner = (s, 2 * z + 1 - c)
    rows, width = hidden.shape
    order = list(range(1, nz)) + [0]
    greet(s, z, c, n_sp, nz)
    halves = {i: send(partial.at[i, 1], rx.at[i], d_send.at[i], d_recv.at[i], partner) for i in order}
    sent = {}
    for i in order:
        halves[i].wait_recv()

        def add(cols, i=i):
            total = partial[i, 0, :, :, cols].astype(jnp.float32) + rx[i, :, :, cols].astype(jnp.float32)
            total = total.astype(jnp.bfloat16)
            stage[i, :, :, cols] = total

        by_columns(width, add)
        sent[i] = [
            send(
                stage.at[i, k], arrived.at[i, k], p_send.at[i, k], p_recv.at[i, k],
                (lax.rem(s + n_sp - k, n_sp), 2 * z + c),
            )
            for k in range(1, n_sp)
        ]
    back = []
    for i in order:
        for copy in sent[i]:
            copy.wait_recv()
        meta = metas[i]
        first, second = slot_hits(meta, s, n_sp, cap)
        weights = jnp.where(first, meta[4:5, :], 0.0) + jnp.where(second, meta[5:6, :], 0.0)
        high = weights.astype(jnp.bfloat16)
        low = (weights - high.astype(jnp.float32)).astype(jnp.bfloat16)

        def combine(cols, i=i, high=high, low=low):
            own = stage[i, 0, :, cols]
            others = [arrived[i, k, :, cols] for k in range(1, n_sp)]
            values = jnp.concatenate([own] + others, axis=0)
            dims = (((0,), (0,)), ((), ()))
            total = lax.dot_general(high, values, dims, preferred_element_type=jnp.float32)
            total = total + lax.dot_general(low, values, dims, preferred_element_type=jnp.float32)
            if i:
                combined[i, :, cols] = total.astype(jnp.bfloat16)
            else:
                mine[:, cols] = total

        by_columns(width, combine)
        if i:
            back.append(
                send(
                    combined.at[i], zrx.at[i], z_send.at[i], z_recv.at[i],
                    (s, 2 * lax.rem(z + nz - i, nz) + c),
                )
            )
    for copy in back:
        copy.wait_recv()

    def finish(r):
        total = mine[r, :]
        for i in range(1, nz):
            total = total + zrx[i, r, :].astype(jnp.float32)
        out[r, :] = (hidden[r, :].astype(jnp.float32) + total).astype(jnp.bfloat16)

    by_rows(rows, finish)
    for copy in list(halves.values()) + sum(sent.values(), []) + back:
        copy.wait_send()


VMEM_LIMIT = 60 * 1024 * 1024


def dispatch(part, residual, gain, meta, n_sp, nz, cap):
    rows, width = residual.shape
    bf16, dma = jnp.bfloat16, pltpu.SemaphoreType.DMA
    vmem = pl.BlockSpec(memory_space=pltpu.VMEM)
    return pl.pallas_call(
        functools.partial(dispatch_kernel, n_sp, nz, cap),
        out_shape=(
            jax.ShapeDtypeStruct((rows, width), bf16),
            jax.ShapeDtypeStruct((nz,) + meta.shape, jnp.float32),
            jax.ShapeDtypeStruct((nz, 2, n_sp, cap, width), bf16),
        ),
        in_specs=[vmem] * 4,
        out_specs=(vmem,) * 3,
        scratch_shapes=[
            pltpu.VMEM((nz, rows, width), bf16),
            pltpu.VMEM((nz, rows, width), bf16),
            pltpu.VMEM((nz, rows, width), bf16),
            pltpu.VMEM((nz, rows, width), bf16),
            pltpu.VMEM((nz, n_sp, cap, width), bf16),
        ]
        + [dma((nz,))] * 8
        + [dma((nz, n_sp))] * 2
        + [dma((nz,))] * 2,
        compiler_params=pltpu.CompilerParams(
            collective_id=0, has_side_effects=True, vmem_limit_bytes=VMEM_LIMIT
        ),
    )(part, residual, gain, meta)


def give_back(partial, hidden, metas, n_sp, nz, cap):
    rows, width = hidden.shape
    bf16, dma = jnp.bfloat16, pltpu.SemaphoreType.DMA
    vmem = pl.BlockSpec(memory_space=pltpu.VMEM)
    return pl.pallas_call(
        functools.partial(return_kernel, n_sp, nz, cap),
        out_shape=jax.ShapeDtypeStruct((rows, width), bf16),
        in_specs=[vmem] * 3,
        out_specs=vmem,
        scratch_shapes=[
            pltpu.VMEM((nz, n_sp, cap, width), bf16),
            pltpu.VMEM((nz, n_sp, cap, width), bf16),
            pltpu.VMEM((nz, n_sp, cap, width), bf16),
            pltpu.VMEM((rows, width), jnp.float32),
            pltpu.VMEM((nz, rows, width), bf16),
            pltpu.VMEM((nz, rows, width), bf16),
        ]
        + [dma((nz,))] * 2
        + [dma((nz, n_sp))] * 2
        + [dma((nz,))] * 2,
        compiler_params=pltpu.CompilerParams(
            collective_id=1, has_side_effects=True, vmem_limit_bytes=VMEM_LIMIT
        ),
    )(partial, hidden, metas)


def describe(expert_ids, route_weights, experts):
    onehot = (expert_ids[:, :, None] == jnp.arange(experts, dtype=jnp.int32)).astype(jnp.float32)
    named = jnp.sum(onehot, axis=1)
    count = named.shape[0]
    before = jnp.arange(count)[:, None] > jnp.arange(count)[None, :]
    earlier = jnp.sum(jnp.where(before[:, :, None], named[None, :, :], 0.0), axis=1)
    slot = jnp.sum(earlier[:, None, :] * onehot, axis=2)
    ids = expert_ids.astype(jnp.float32)
    zero = jnp.zeros_like(slot[:, 0])
    return jnp.stack(
        [ids[:, 0], slot[:, 0], ids[:, 1], slot[:, 1], route_weights[:, 0], route_weights[:, 1], zero, zero]
    )


def shards(
    out_gate,
    in_gate,
    conv_input,
    conv_taps,
    documents,
    out_weight,
    residual,
    norm_gain,
    expert_ids,
    route_weights,
    gate_weight,
    up_weight,
    down_weight,
):
    length = conv_input.shape[0]
    signal = in_gate.astype(jnp.float32) * conv_input.astype(jnp.float32)
    doc_values = documents.astype(jnp.float32)
    prior_signal, prior_docs = passed_along(
        (signal[length - 2 :], doc_values[length - 2 :]), "sp", 1
    )
    long_signal = jnp.concatenate([prior_signal, signal], axis=0)
    long_docs = jnp.concatenate([prior_docs, doc_values], axis=0)
    position = lax.axis_index("sp") * length + jnp.arange(length, dtype=jnp.int32)
    tap_values = conv_taps.astype(jnp.float32)
    mixed_conv = tap_values[2][None, :] * signal
    for offset in (1, 2):
        earlier_signal = long_signal[2 - offset : 2 - offset + length]
        earlier_docs = long_docs[2 - offset : 2 - offset + length]
        allowed = (position >= offset) & (earlier_docs == doc_values)
        mixed_conv = mixed_conv + jnp.where(
            allowed[:, None], tap_values[2 - offset][None, :] * earlier_signal, 0.0
        )
    gated = (out_gate.astype(jnp.float32) * mixed_conv).astype(jnp.bfloat16)
    block_rows = length // lax.axis_size("tp")
    n_sp, nz = lax.axis_size("sp"), lax.axis_size("tp") // 2
    width = residual.shape[1]
    capacity = max(2, (3 * block_rows + n_sp - 1) // n_sp)
    cap = -(-capacity // CHUNK) * CHUNK
    meta = describe(expert_ids, route_weights, n_sp)
    part = jnp.dot(gated, out_weight, preferred_element_type=jnp.float32).astype(jnp.bfloat16)
    hidden, metas, gathered = dispatch(
        part.reshape(nz, 2, block_rows, width), residual, norm_gain[None, :], meta, n_sp, nz, cap
    )
    rows = gathered.reshape(-1, width)
    gate_proj = jnp.dot(rows, gate_weight[0], preferred_element_type=jnp.float32)
    up_proj = jnp.dot(rows, up_weight[0], preferred_element_type=jnp.float32)
    act = (jax.nn.silu(gate_proj) * up_proj).astype(jnp.bfloat16)
    partial = jnp.dot(act, down_weight[0], preferred_element_type=jnp.float32).astype(jnp.bfloat16)
    return give_back(partial.reshape(gathered.shape), hidden, metas, n_sp, nz, cap)


def solution(mesh):
    in_specs = (
        P("sp", "tp"),
        P("sp", "tp"),
        P("sp", "tp"),
        P(None, "tp"),
        P("sp"),
        P("tp", None),
        P(("sp", "tp"), None),
        P(),
        P(("sp", "tp"), None),
        P(("sp", "tp"), None),
        P("sp", None, "tp"),
        P("sp", None, "tp"),
        P("sp", "tp", None),
    )
    out_specs = P(("sp", "tp"), None)
    return jax.shard_map(shards, mesh=mesh, in_specs=in_specs, out_specs=out_specs, check_vma=False)
```

```python
import functools

import jax
import jax.numpy as jnp
from jax import lax
from jax.experimental import pallas as pl
from jax.experimental.pallas import tpu as pltpu
from jax.sharding import PartitionSpec as P

EPS = 1e-06


MESH = pl.DeviceIdType.MESH
CHUNK = 16
COLS = 512
UNITS = 256
HALO = 8
STRIP = 64
LANES = 128
VMEM_LIMIT = 63 * 1024 * 1024


def where_am_i(n_sp, nz):
    s, t = lax.axis_index("sp"), lax.axis_index("tp")
    z, c = t // 2, t % 2
    return s, z, c


def greet(s, z, c, n_sp, nz):
    barrier = pltpu.get_barrier_semaphore()
    peers = [(s, 2 * z + 1 - c)]
    peers += [(s, 2 * lax.rem(z + i, nz) + c) for i in range(1, nz)]
    peers += [(lax.rem(s + k, n_sp), 2 * z + c) for k in range(1, n_sp)]
    for peer in peers:
        pl.semaphore_signal(barrier, inc=1, device_id=peer, device_id_type=MESH)
    return lambda: pl.semaphore_wait(barrier, len(peers))


def send(src, dst, send_sem, recv_sem, peer):
    copy = pltpu.make_async_remote_copy(
        src_ref=src,
        dst_ref=dst,
        send_sem=send_sem,
        recv_sem=recv_sem,
        device_id=peer,
        device_id_type=MESH,
    )
    copy.start()
    return copy


def by_rows(rows, body):
    def step(r, carry):
        body(pl.ds(pl.multiple_of(r * CHUNK, CHUNK), CHUNK))
        return carry

    lax.fori_loop(0, rows // CHUNK, step, 0)


def by_columns(width, body):
    def step(r, carry):
        body(pl.ds(pl.multiple_of(r * COLS, COLS), COLS))
        return carry

    lax.fori_loop(0, width // COLS, step, 0)


def slot_hits(meta, s, n_sp, cap):
    rows = meta.shape[1]
    slots = lax.broadcasted_iota(jnp.int32, (n_sp * cap, rows), 0).astype(jnp.float32)
    own = s.astype(jnp.float32)
    hits = []
    for k in range(2):
        ahead = meta[2 * k : 2 * k + 1, :] - own
        ahead = jnp.where(ahead < 0.0, ahead + float(n_sp), ahead)
        hits.append(slots == ahead * float(cap) + meta[2 * k + 1 : 2 * k + 2, :])
    return hits


def describe(routes, meta, n_sp):
    rows = routes.shape[1]
    choice = [routes[0:1, :], routes[1:2, :]]
    expert = lax.broadcasted_iota(jnp.int32, (-(-n_sp // CHUNK) * CHUNK, rows), 0).astype(jnp.float32)
    names = [expert == choice[0], expert == choice[1]]
    named = (names[0] | names[1]).astype(jnp.float32).astype(jnp.bfloat16)
    before = lax.broadcasted_iota(jnp.int32, (rows, rows), 0) < lax.broadcasted_iota(jnp.int32, (rows, rows), 1)
    earlier = jnp.dot(
        named, before.astype(jnp.float32).astype(jnp.bfloat16), preferred_element_type=jnp.float32
    )
    for k in range(2):
        meta[2 * k : 2 * k + 1, :] = choice[k]
        meta[2 * k + 1 : 2 * k + 2, :] = jnp.sum(jnp.where(names[k], earlier, 0.0), axis=0, keepdims=True)
    meta[4:6, :] = routes[2:4, :]
    meta[6:8, :] = jnp.zeros((2, rows), jnp.float32)


def layer_kernel(
    n_sp, nz, cap,
    in_gate, conv_input, out_gate, taps, docs, out_weight, residual, gain, routes, gate_hbm, up_hbm, down_hbm,
    out,
    gate, up, down, signal, long_docs, tail_signal, tail_docs, halo_signal, halo_docs, gated, part, meta, metas,
    hidden, rx, stage, rz, nbuf, routed, gathered, act, half_rx, arrived, mine, combined, zrx,
    w_sem, h_send, h_recv,
    d_send, d_recv, m_send, m_recv, z_send, z_recv, n_send, n_recv, p_send, p_recv, f_send, f_recv,
    e_send, e_recv, r_send, r_recv, b_send, b_recv,
):
    s, z, c = where_am_i(n_sp, nz)
    o = 1 - c
    partner = (s, 2 * z + o)
    rows, width = residual.shape
    length, channels = in_gate.shape
    order = list(range(1, nz)) + [0]
    ahead = [lax.rem(z + i, nz) for i in range(nz)]
    greeted = greet(s, z, c, n_sp, nz)
    loads = [
        pltpu.make_async_copy(src, dst, w_sem.at[i])
        for i, (src, dst) in enumerate([(gate_hbm, gate), (up_hbm, up), (down_hbm, down)])
    ]
    for load in loads:
        load.start()

    tail = slice(length - HALO, length)
    tail_signal[...] = in_gate[tail, :].astype(jnp.float32) * conv_input[tail, :].astype(jnp.float32)
    tail_docs[...] = docs[tail, :]
    signal[HALO:, :] = in_gate[...].astype(jnp.float32) * conv_input[...].astype(jnp.float32)
    long_docs[HALO:, :] = docs[...]
    describe(routes, meta, n_sp)
    metas[0] = meta[...]
    greeted()
    following = (lax.rem(s + 1, n_sp), 2 * z + c)
    halo = [
        send(tail_signal, halo_signal, h_send.at[0], h_recv.at[0], following),
        send(tail_docs, halo_docs, h_send.at[1], h_recv.at[1], following),
    ]
    for copy in halo:
        copy.wait_recv()
    signal[:HALO, :] = halo_signal[...]
    long_docs[:HALO, :] = jnp.where(s == 0, -1.0, halo_docs[...])
    tap_values = taps[...].astype(jnp.float32)
    for r in range(0, length, STRIP):
        at = [slice(HALO + r - j, HALO + r - j + STRIP) for j in range(3)]
        here = long_docs[at[0], :]
        same = [None] + [long_docs[at[j], :] == here for j in (1, 2)]
        for l in range(0, channels, LANES):
            lane = slice(l, l + LANES)
            conv = tap_values[2:3, lane] * signal[at[0], lane]
            for j in (1, 2):
                conv = conv + jnp.where(same[j], tap_values[2 - j : 3 - j, lane] * signal[at[j], lane], 0.0)
            gated[r : r + STRIP, lane] = (out_gate[r : r + STRIP, lane].astype(jnp.float32) * conv).astype(
                jnp.bfloat16
            )

    def project(cols):
        part[:, cols] = jnp.dot(
            gated[...], out_weight[:, cols], preferred_element_type=jnp.float32
        ).astype(jnp.bfloat16)

    by_columns(width, project)

    def block(at_z, core):
        return pl.multiple_of((2 * at_z + core) * rows, rows)

    halves = {}
    for i in order:
        halves[i] = send(
            part.at[pl.ds(block(ahead[i], o), rows)], rx.at[i], d_send.at[i], d_recv.at[i], partner
        )
    notes = [send(meta, metas.at[i], m_send.at[i], m_recv.at[i], (s, 2 * ahead[i] + c)) for i in range(1, nz)]
    sums = []
    for i in order:
        halves[i].wait_recv()
        if i:

            def add(r, i=i):
                own = part[pl.ds(pl.multiple_of(block(ahead[i], c) + r.start, CHUNK), CHUNK), :]
                stage[i, r, :] = (own.astype(jnp.float32) + rx[i, r, :].astype(jnp.float32)).astype(jnp.bfloat16)

            by_rows(rows, add)
            sums.append(send(stage.at[i], rz.at[i], z_send.at[i], z_recv.at[i], (s, 2 * ahead[i] + c)))
    for copy in sums:
        copy.wait_recv()

    def norm(r):
        own = part[pl.ds(pl.multiple_of(block(z, c) + r.start, CHUNK), CHUNK), :]
        total = own.astype(jnp.float32) + rx[0, r, :].astype(jnp.float32)
        for i in range(1, nz):
            total = total + rz[i, r, :].astype(jnp.float32)
        state = (residual[r, :].astype(jnp.float32) + total).astype(jnp.bfloat16)
        hidden[r, :] = state
        wide = state.astype(jnp.float32)
        stats = jnp.mean(wide * wide, axis=-1, keepdims=True)
        nbuf[0, r, :] = (wide * lax.rsqrt(stats + EPS) * gain[...].astype(jnp.float32)).astype(jnp.bfloat16)

    by_rows(rows, norm)
    spread = [
        send(nbuf.at[0], nbuf.at[i], n_send.at[i], n_recv.at[i], (s, 2 * ahead[i] + c)) for i in range(1, nz)
    ]

    sent, forwards, swaps, returns, back = {}, {}, {}, {}, []

    def build(i):
        if i:
            notes[i - 1].wait_recv()
            spread[i - 1].wait_recv()
        first, second = slot_hits(metas[i], s, n_sp, cap)
        table = (first | second).astype(jnp.float32).astype(jnp.bfloat16)

        def place(cols):
            placed = jnp.dot(table, nbuf[i, :, cols], preferred_element_type=jnp.float32).astype(jnp.bfloat16)
            gathered[i, 0, 0, :, cols] = placed[:cap]
            for k in range(1, n_sp):
                routed[i, k, :, cols] = placed[k * cap : (k + 1) * cap]

        by_columns(width, place)
        sent[i] = [
            send(
                routed.at[i, k], gathered.at[i, 0, k], p_send.at[i, k], p_recv.at[i, k],
                (lax.rem(s + k, n_sp), 2 * z + c),
            )
            for k in range(1, n_sp)
        ]

    def forward(i):
        for copy in sent[i]:
            copy.wait_recv()
        forwards[i] = send(gathered.at[i, 0], gathered.at[i, 1], f_send.at[i], f_recv.at[i], partner)

    def expert(i):
        if i == 0:
            for load in loads:
                load.wait()
        forwards[i].wait_recv()
        half = n_sp * cap
        hidden_units = gate.shape[1]
        step = min(UNITS, hidden_units)

        def inner(r, carry):
            units = pl.ds(pl.multiple_of(r * step, step), step)
            held = gathered[i].reshape(2 * half, width)
            gate_proj = jnp.dot(held, gate[:, units], preferred_element_type=jnp.float32)
            up_proj = jnp.dot(held, up[:, units], preferred_element_type=jnp.float32)
            act[:, units] = (gate_proj / (1.0 + jnp.exp(-gate_proj)) * up_proj).astype(jnp.bfloat16)
            return carry

        lax.fori_loop(0, hidden_units // step, inner, 0)
        for copy in sent[i]:
            copy.wait_send()
        forwards[i].wait_send()

        def outer(cols):
            share = jnp.dot(act[...], down[:, cols], preferred_element_type=jnp.float32).astype(jnp.bfloat16)
            routed[i, :, :, cols] = share[:half].reshape(n_sp, cap, COLS)
            gathered[i, 0, :, :, cols] = share[half:].reshape(n_sp, cap, COLS)

        by_columns(width, outer)
        swaps[i] = send(gathered.at[i, 0], half_rx.at[i], e_send.at[i], e_recv.at[i], partner)

    def give_back(i):
        swaps[i].wait_recv()

        def add(cols):
            total = routed[i, :, :, cols].astype(jnp.float32) + half_rx[i, :, :, cols].astype(jnp.float32)
            routed[i, :, :, cols] = total.astype(jnp.bfloat16)

        by_columns(width, add)
        returns[i] = [
            send(
                routed.at[i, k], arrived.at[i, k], r_send.at[i, k], r_recv.at[i, k],
                (lax.rem(s + n_sp - k, n_sp), 2 * z + c),
            )
            for k in range(1, n_sp)
        ]

    def combine(i):
        for copy in returns[i]:
            copy.wait_recv()
        weight_rows = metas[i]
        first, second = slot_hits(weight_rows, s, n_sp, cap)
        weights = jnp.where(first, weight_rows[4:5, :], 0.0) + jnp.where(second, weight_rows[5:6, :], 0.0)
        high = weights.astype(jnp.bfloat16)
        low = (weights - high.astype(jnp.float32)).astype(jnp.bfloat16)

        def weigh(cols):
            values = jnp.concatenate(
                [routed[i, 0, :, cols]] + [arrived[i, k, :, cols] for k in range(1, n_sp)], axis=0
            )
            dims = (((0,), (0,)), ((), ()))
            total = lax.dot_general(high, values, dims, preferred_element_type=jnp.float32)
            total = total + lax.dot_general(low, values, dims, preferred_element_type=jnp.float32)
            if i:
                combined[i, :, cols] = total.astype(jnp.bfloat16)
            else:
                mine[:, cols] = total

        by_columns(width, weigh)
        if i:
            back.append(
                send(
                    combined.at[i], zrx.at[i], b_send.at[i], b_recv.at[i], (s, 2 * lax.rem(z + nz - i, nz) + c)
                )
            )

    for i in range(nz):
        build(i)
        if i >= 1:
            forward(i - 1)
        if i >= 2:
            expert(i - 2)
            if i >= 3:
                give_back(i - 2)
    forward(nz - 1)
    for i in range(max(nz - 2, 0), nz):
        expert(i)
        if i:
            give_back(i)
    give_back(0)
    for i in order:
        combine(i)
    for copy in back:
        copy.wait_recv()

    def finish(r):
        total = mine[r, :]
        for i in range(1, nz):
            total = total + zrx[i, r, :].astype(jnp.float32)
        out[r, :] = (hidden[r, :].astype(jnp.float32) + total).astype(jnp.bfloat16)

    by_rows(rows, finish)
    left = halo + list(halves.values()) + notes + sums + spread + list(swaps.values()) + back
    for copy in left + sum(returns.values(), []):
        copy.wait_send()


def shards(
    out_gate,
    in_gate,
    conv_input,
    conv_taps,
    documents,
    out_weight,
    residual,
    norm_gain,
    expert_ids,
    route_weights,
    gate_weight,
    up_weight,
    down_weight,
):
    n_sp, nz = lax.axis_size("sp"), lax.axis_size("tp") // 2
    length, channels = conv_input.shape
    rows, width = residual.shape
    units = gate_weight.shape[2]
    capacity = max(2, (3 * rows + n_sp - 1) // n_sp)
    cap = -(-capacity // CHUNK) * CHUNK
    docs = jnp.broadcast_to(documents.astype(jnp.float32)[:, None], (length, LANES))
    routes = jnp.concatenate([expert_ids.astype(jnp.float32).T, route_weights.T], axis=0)
    bf16, f32, dma = jnp.bfloat16, jnp.float32, pltpu.SemaphoreType.DMA
    vmem, hbm = pl.BlockSpec(memory_space=pltpu.VMEM), pl.BlockSpec(memory_space=pltpu.HBM)
    per_z = pltpu.VMEM((nz, rows, width), bf16)
    slots = pltpu.VMEM((nz, n_sp, cap, width), bf16)
    return pl.pallas_call(
        functools.partial(layer_kernel, n_sp, nz, cap),
        out_shape=jax.ShapeDtypeStruct((rows, width), bf16),
        in_specs=[vmem] * 9 + [hbm] * 3,
        out_specs=vmem,
        scratch_shapes=[
            pltpu.VMEM((width, units), bf16),
            pltpu.VMEM((width, units), bf16),
            pltpu.VMEM((units, width), bf16),
            pltpu.VMEM((HALO + length, channels), f32),
            pltpu.VMEM((HALO + length, LANES), f32),
            pltpu.VMEM((HALO, channels), f32),
            pltpu.VMEM((HALO, LANES), f32),
            pltpu.VMEM((HALO, channels), f32),
            pltpu.VMEM((HALO, LANES), f32),
            pltpu.VMEM((length, channels), bf16),
            pltpu.VMEM((length, width), bf16),
            pltpu.VMEM((8, rows), f32),
            pltpu.VMEM((nz, 8, rows), f32),
            pltpu.VMEM((rows, width), bf16),
            per_z,
            per_z,
            per_z,
            per_z,
            slots,
            pltpu.VMEM((nz, 2, n_sp, cap, width), bf16),
            pltpu.VMEM((2 * n_sp * cap, units), bf16),
            slots,
            slots,
            pltpu.VMEM((rows, width), f32),
            per_z,
            per_z,
            dma((3,)),
            dma((2,)),
            dma((2,)),
        ]
        + [dma((nz,))] * 8
        + [dma((nz, n_sp))] * 2
        + [dma((nz,))] * 4
        + [dma((nz, n_sp))] * 2
        + [dma((nz,))] * 2,
        compiler_params=pltpu.CompilerParams(
            collective_id=0, has_side_effects=True, vmem_limit_bytes=VMEM_LIMIT
        ),
    )(
        in_gate, conv_input, out_gate, conv_taps, docs, out_weight, residual, norm_gain[None, :], routes,
        gate_weight[0], up_weight[0], down_weight[0],
    )


def solution(mesh):
    in_specs = (
        P("sp", "tp"),
        P("sp", "tp"),
        P("sp", "tp"),
        P(None, "tp"),
        P("sp"),
        P("tp", None),
        P(("sp", "tp"), None),
        P(),
        P(("sp", "tp"), None),
        P(("sp", "tp"), None),
        P("sp", None, "tp"),
        P("sp", None, "tp"),
        P("sp", "tp", None),
    )
    out_specs = P(("sp", "tp"), None)
    return jax.shard_map(shards, mesh=mesh, in_specs=in_specs, out_specs=out_specs, check_vma=False)
```
